256 devices in a mesh: grp: 2 (over y), ep: 32 (over z, core), tp: 4 (over x).
Axes of the slice: x: 4, y: 2, z: 16, core: 2. Of those that a mesh axis runs over, the one named last changes fastest.
The devices are a block of a 4x16x16 slice.
Arguments:
- query_first: bfloat16 [24576, 512], P(('grp', 'ep'), 'tp'), parts along dimension 0, may hold values from -32 to 32
- query_second: bfloat16 [24576, 512], P(('grp', 'ep'), 'tp'), parts along dimension 0, may hold values from -32 to 32
- key_first: bfloat16 [24576, 512], P(('grp', 'ep'), 'tp'), parts along dimension 0, may hold values from -32 to 32
- key_second: bfloat16 [24576, 512], P(('grp', 'ep'), 'tp'), parts along dimension 0, may hold values from -32 to 32
- values: bfloat16 [24576, 1024], P(('grp', 'ep'), 'tp'), parts along dimension 0, may hold values from -6 to 6
- lambda_head: float32 [8], P('tp'), may hold values from 0.3 to 0.8
- head_gain: float32 [128], replicated, may hold values from 0.1 to 1.9
- out_weight: bfloat16 [1024, 2048], replicated, may hold values from -0.1875 to 0.1875
- tokens: bfloat16 [32768, 2048], P(('grp', 'ep', 'tp')), parts along dimension 0, may hold values from -6 to 6
- norm_gain: float32 [2048], replicated, may hold values from 0.1 to 1.9
- expert_ids: int32 [32768, 2], P(('grp', 'ep', 'tp')), parts along dimension 0, may hold values from 0 to 31, all different within a row; in each aligned block of 128 rows (0 to 127, 128 to 255, ...) at most 12 rows name the same one
- expert_weights: float32 [32768, 2], P(('grp', 'ep', 'tp')), parts along dimension 0, may hold values from 0.2 to 1
- expert_gate: bfloat16 [32, 2048, 1024], P('ep', None, 'tp'), may hold values from -0.125 to 0.125
- expert_up: bfloat16 [32, 2048, 1024], P('ep', None, 'tp'), may hold values from -0.125 to 0.125
- expert_down: bfloat16 [32, 1024, 2048], P('ep', 'tp'), may hold values from -0.1875 to 0.1875
- shared_gate: bfloat16 [2048, 512], P(None, 'tp'), may hold values from -0.125 to 0.125
- shared_up: bfloat16 [2048, 512], P(None, 'tp'), may hold values from -0.125 to 0.125
- shared_down: bfloat16 [512, 2048], P('tp'), may hold values from -0.25 to 0.25
Outputs:
- mixed: bfloat16 [24576, 2048], P(('grp', 'ep', 'tp')), parts along dimension 0
- expert_out: bfloat16 [32768, 2048], P(('grp', 'ep', 'tp')), parts along dimension 0
The draws below stay inside these ranges and needn't reach their ends.
There are 2 independent parts, one for each index of `grp`. The reference program is written for one: setup_inputs(seed, part) draws one part's arguments, and reference() takes and returns one part's arrays. A program takes and returns all parts, laid end to end along the dimension named above; an argument that names none is the same for every part. Nothing has to cross between parts.
Inputs may be any that keep to these rules, and one draw needn't show every extreme that they name: `expert_ids`: in the rows of one device (aligned blocks of 128 rows) no expert is named by more than 12 rows, and in every draw some expert is named by exactly 12 rows of some block; each row names 2 different experts.
All inputs are finite; a program needn't handle non-finite values.
Results may differ from the reference program's by a relative error of at most 0.012.
Values may be sent and summed in bfloat16 or wider, within the bound.
A program may use at most 128 MiB of HBM per device.

```python
import math
import jax
import jax.numpy as jnp
import numpy as np
from jax import lax

D = 2048
HEADS = 8
HEAD = 64
VDIM = 128
FF = 1024
SHARED = 512
TOPK = 2
ROW_DEV = 128
TOKENS_A = 12288
TOKENS_E = 16384
EXPERTS = 32
CAP = 12
N_TP = 4


def drawn_pair(key, which):
    base = jax.random.fold_in(key, 4100 + which)
    key_query, key_keys = jax.random.split(base, 2)
    shape = (TOKENS_A, HEADS * HEAD)
    queries = 1.3 * jax.random.truncated_normal(key_query, -3.8, 3.8, shape, jnp.float32)
    keys = 1.3 * jax.random.truncated_normal(key_keys, -3.8, 3.8, shape, jnp.float32)
    return (queries.astype(jnp.bfloat16), keys.astype(jnp.bfloat16))


def draw_query_first(key, part):
    return drawn_pair(key, 0)[0]


def draw_key_first(key, part):
    return drawn_pair(key, 0)[1]


def draw_query_second(key, part):
    return drawn_pair(key, 1)[0]


def draw_key_second(key, part):
    return drawn_pair(key, 1)[1]


def steps_of(key, dims, cuts, smallest, largest):
    level = 1.0
    for dim, parts in cuts:
        heights = jax.random.uniform(jax.random.fold_in(jax.random.fold_in(key, 6), dim), (parts,), jnp.float32, smallest / len(cuts), largest / len(cuts))
        level = level * jnp.repeat(jnp.exp(heights), dims[dim] // parts).reshape((-1,) + (1,) * (len(dims) - 1 - dim))
    return level


def deal_out(key, own, number, rows, number_of, top, bound, slope):
    sequence = jax.random.permutation(key, number_of)
    heavy_load, ordinary = portions_of(number_of, rows * top, bound, slope, True), portions_of(number_of, rows * top, bound, slope, False)
    places = jnp.arange(number_of)

    def named(lengths, turn):
        used = int((lengths > 0).sum())
        fixed = max(1, used // 4)
        shifted = fixed + (places - fixed + turn * (used - fixed)) % max(1, number_of - fixed)
        return jnp.zeros((number_of,), jnp.int32).at[sequence[jnp.where(places < fixed, places, shifted)]].set(jnp.asarray(lengths, jnp.int32))

    lengths = jnp.where(number % 4 == 0, named(heavy_load, number // 4), named(ordinary, number - number // 4 - 1))
    mixed = jax.random.permutation(jax.random.fold_in(own, 3), number_of)
    donor, receiver = mixed[0:number_of // 2 * 2:2], mixed[1:number_of // 2 * 2:2]
    slack = jnp.minimum(lengths[donor] - 1, bound - lengths[receiver]) // 2
    slack = jnp.where((donor == sequence[0]) | (receiver == sequence[0]) | (lengths[receiver] == 0), 0, jnp.maximum(slack, 0))
    shifted = jax.random.randint(jax.random.fold_in(own, 4), (number_of // 2,), 0, 1 << 20) % (slack + 1)
    lengths = lengths.at[donor].add(-shifted).at[receiver].add(shifted)
    items = jnp.searchsorted(jnp.cumsum(lengths), jnp.arange(rows * top), side="right").astype(jnp.int32)
    grid = items.reshape(top, rows).T
    grid = grid[jax.random.permutation(jax.random.fold_in(own, 1), rows)]
    turn = jax.random.randint(jax.random.fold_in(own, 2), (rows, 1), 0, top)
    return jnp.take_along_axis(grid, (jnp.arange(top)[None, :] + turn) % top, axis=1)


def portions_of(number_of, total, most, skew, full):
    portions = [(1 << 20) // math.isqrt(rank ** skew) + 1 for rank in range(1, number_of + 1)]
    largest = most if full else min(most, max(-(-total // number_of), total * portions[0] // sum(portions)))
    least = 1 if total - largest >= number_of - 1 else 0
    counts, rest = [largest] + [least] * (number_of - 1), total - largest - least * (number_of - 1)
    while rest > 0:
        movable = [i for i in range(1, number_of) if counts[i] < largest] or [i for i in range(1, number_of) if counts[i] < most]
        whole, budget = sum([portions[i] for i in movable]), rest
        for i in movable:
            addition = min(most - counts[i], max(1, budget * portions[i] // whole), rest)
            counts[i] = counts[i] + addition
            rest = rest - addition
    return np.array(counts)


def centred(stream_key, shape, scale, limit, shards=(), held_as=jnp.bfloat16):
    drawn = jax.random.normal(stream_key, shape, jnp.float32) * scale
    if len(shards) > 0:
        drawn = steps_of(stream_key, shape, shards, -0.22, 0.18) * drawn
    return jnp.clip(drawn, min=-limit, max=limit).astype(held_as)


def setup_inputs(seed: int = 0, part: int = 0) -> dict:
    streams_of = jax.random.split(jax.random.key(seed), 19)
    part_keys = jax.random.split(jax.random.fold_in(streams_of[18], part), 19)
    query_first = draw_query_first(jax.random.fold_in(jax.random.fold_in(streams_of[18], part), 71), part)
    query_second = draw_query_second(jax.random.fold_in(jax.random.fold_in(streams_of[18], part), 71), part)
    key_first = draw_key_first(jax.random.fold_in(jax.random.fold_in(streams_of[18], part), 71), part)
    key_second = draw_key_second(jax.random.fold_in(jax.random.fold_in(streams_of[18], part), 71), part)
    values = centred(part_keys[4], (TOKENS_A, HEADS * VDIM), 1.0, 6.0, ((0, 32), (1, 4)))
    lambda_head = jnp.clip(0.3 + 0.5 * jax.random.uniform(streams_of[5], (HEADS,), jnp.float32) ** steps_of(streams_of[5], (HEADS,), ((0, 4),), -0.2, 0.2), 0.3, 0.8)
    head_gain = jnp.clip(1.0 + 0.18 * jax.random.normal(streams_of[6], (VDIM,), jnp.float32), 0.1, 1.9)
    out_weight = centred(streams_of[7], (HEADS * VDIM, D), (HEADS * VDIM) ** -0.5, 0.1875)
    tokens = centred(part_keys[8], (TOKENS_E, D), 1.0, 6.0, ((0, 128),))
    norm_gain = jnp.clip(1.0 + 0.18 * jax.random.normal(streams_of[9], (D,), jnp.float32), 0.1, 1.9)
    expert_ids_keys = jax.random.split(jax.random.fold_in(part_keys[10], 1), TOKENS_E // ROW_DEV)
    expert_ids_turns = jax.random.permutation(jax.random.fold_in(part_keys[10], 3), TOKENS_E // ROW_DEV)
    expert_ids = jax.vmap(lambda own, number: deal_out(jax.random.fold_in(part_keys[10], 2), own, number, ROW_DEV, EXPERTS, TOPK, CAP, 1))(expert_ids_keys, expert_ids_turns).reshape((TOKENS_E, TOPK))
    expert_weights = jnp.clip(0.2 + 0.8 * jax.random.uniform(part_keys[11], (TOKENS_E, TOPK), jnp.float32) ** steps_of(part_keys[11], (TOKENS_E, TOPK), ((0, 128),), -0.2, 0.2), 0.2, 1.0)
    expert_gate = centred(streams_of[12], (EXPERTS, D, FF), D ** -0.5, 0.125, ((0, 32), (2, 4)))
    expert_up = centred(streams_of[13], (EXPERTS, D, FF), D ** -0.5, 0.125, ((0, 32), (2, 4)))
    expert_down = centred(streams_of[14], (EXPERTS, FF, D), FF ** -0.5, 0.1875, ((0, 32), (1, 4)))
    shared_gate = centred(streams_of[15], (D, SHARED), D ** -0.5, 0.125, ((1, 4),))
    shared_up = centred(streams_of[16], (D, SHARED), D ** -0.5, 0.125, ((1, 4),))
    shared_down = centred(streams_of[17], (SHARED, D), SHARED ** -0.5, 0.25, ((0, 4),))
    return {"query_first": query_first, "query_second": query_second, "key_first": key_first, "key_second": key_second, "values": values, "lambda_head": lambda_head, "head_gain": head_gain, "out_weight": out_weight, "tokens": tokens, "norm_gain": norm_gain, "expert_ids": expert_ids, "expert_weights": expert_weights, "expert_gate": expert_gate, "expert_up": expert_up, "expert_down": expert_down, "shared_gate": shared_gate, "shared_up": shared_up, "shared_down": shared_down}


epsilon = 1e-06

def reference(query_first, query_second, key_first, key_second, values, lambda_head, head_gain, out_weight, tokens, norm_gain, expert_ids, expert_weights, expert_gate, expert_up, expert_down, shared_gate, shared_up, shared_down):
    score_scale = HEAD ** (-0.5)
    key_one = key_first.astype(jnp.float32).reshape(TOKENS_A, HEADS, HEAD)
    key_two = key_second.astype(jnp.float32).reshape(TOKENS_A, HEADS, HEAD)
    value_all = values.astype(jnp.float32).reshape(TOKENS_A, HEADS, VDIM)
    query_rows = math.gcd(TOKENS_A, 256)

    def one_map(queries, keys):
        scores = jnp.einsum('qhd,khd->qhk', queries, keys) * score_scale
        row_peak = lax.optimization_barrier(jnp.max(scores, axis=-1, keepdims=True))
        exponent = jnp.exp(scores - row_peak)
        row_total = lax.optimization_barrier(jnp.sum(exponent, axis=-1))
        rounded = lax.optimization_barrier(exponent.astype(jnp.bfloat16)).astype(jnp.float32)
        return jnp.einsum('qhk,khe->qhe', rounded, value_all) / row_total[..., None]

    def query_block(query_pair):
        first_block, second_block = query_pair
        mixture = one_map(first_block, key_one) - lambda_head[None, :, None] * one_map(second_block, key_two)
        normed_heads = mixture * lax.rsqrt(lax.optimization_barrier(jnp.mean(mixture * mixture, axis=-1, keepdims=True)) + epsilon) * head_gain
        return normed_heads.astype(jnp.bfloat16)
    query_one = query_first.astype(jnp.float32).reshape(TOKENS_A // query_rows, query_rows, HEADS, HEAD)
    query_two = query_second.astype(jnp.float32).reshape(TOKENS_A // query_rows, query_rows, HEADS, HEAD)
    head_rows = lax.map(query_block, (query_one, query_two)).reshape(TOKENS_A, HEADS * VDIM)
    mixed = jnp.dot(head_rows, out_weight, preferred_element_type=jnp.float32).astype(jnp.bfloat16)
    widened = tokens.astype(jnp.float32)
    normed = (widened * lax.rsqrt(lax.optimization_barrier(jnp.mean(widened * widened, axis=-1, keepdims=True)) + epsilon) * norm_gain).astype(jnp.bfloat16)
    block_count = TOKENS_E // ROW_DEV
    copies = ROW_DEV * TOPK
    chosen = expert_ids.reshape(block_count, copies)
    onehot = (chosen[:, :, None] == jnp.arange(EXPERTS, dtype=jnp.int32)[None, None, :]).astype(jnp.int32)
    rank_in_block = lax.optimization_barrier(jnp.sum(onehot * jnp.cumsum(onehot, axis=1), axis=-1)) - 1
    block_index = jnp.arange(block_count, dtype=jnp.int32)[:, None]
    slot_index = (chosen * (block_count * CAP) + block_index * CAP + rank_in_block).reshape(-1)
    token_index = (block_index * ROW_DEV + jnp.arange(copies, dtype=jnp.int32)[None, :] // TOPK).reshape(-1)
    slot_tokens = jnp.full((EXPERTS * block_count * CAP,), TOKENS_E, jnp.int32).at[slot_index].set(token_index)
    slot_tokens = slot_tokens.reshape(EXPERTS, block_count * CAP)
    slot_weights = jnp.zeros((EXPERTS * block_count * CAP,), jnp.float32).at[slot_index].set(expert_weights.reshape(-1))
    slot_weights = slot_weights.reshape(EXPERTS, block_count * CAP)
    padded = jnp.concatenate([normed, jnp.zeros((1, D), jnp.bfloat16)], axis=0)

    def expert_step(accum, inputs):
        index_rows, weight_rows, gate_matrix, up_matrix, down_matrix = inputs
        picked = padded[index_rows]
        gate_value = jnp.dot(picked, gate_matrix, preferred_element_type=jnp.float32)
        up_value = jnp.dot(picked, up_matrix, preferred_element_type=jnp.float32)
        hidden = (jax.nn.silu(gate_value) * up_value).astype(jnp.bfloat16)
        grouped = hidden.astype(jnp.float32).reshape(-1, N_TP, FF // N_TP)
        down_groups = down_matrix.astype(jnp.float32).reshape(N_TP, FF // N_TP, D)
        partial_value = jnp.einsum('mjf,jfd->jmd', grouped, down_groups)
        rounded = lax.optimization_barrier(partial_value.astype(jnp.bfloat16)).astype(jnp.float32)
        routed = lax.optimization_barrier(lax.optimization_barrier(jnp.sum(rounded, axis=0)).astype(jnp.bfloat16)).astype(jnp.float32)
        return (accum.at[index_rows].add(routed * weight_rows[:, None]), None)
    accum_start = jnp.zeros((TOKENS_E + 1, D), jnp.float32)
    routed_sum, unused = lax.scan(expert_step, accum_start, (slot_tokens, slot_weights, expert_gate, expert_up, expert_down))
    group_width = SHARED // N_TP
    shared_part = jnp.zeros((TOKENS_E, D), jnp.float32)
    for quarter in range(N_TP):
        columns = slice(quarter * group_width, (quarter + 1) * group_width)
        gate_value = jnp.dot(normed, shared_gate[:, columns], preferred_element_type=jnp.float32)
        up_value = jnp.dot(normed, shared_up[:, columns], preferred_element_type=jnp.float32)
        shared_hidden = (jax.nn.silu(gate_value) * up_value).astype(jnp.bfloat16)
        partial_value = jnp.dot(shared_hidden, shared_down[columns, :], preferred_element_type=jnp.float32)
        shared_part = shared_part + lax.optimization_barrier(partial_value.astype(jnp.bfloat16)).astype(jnp.float32)
    expert_out = (routed_sum[:TOKENS_E] + shared_part).astype(jnp.bfloat16)
    return (mixed, expert_out)
```

```python
import functools

import jax
import jax.numpy as jnp
from jax import lax
from jax.experimental import pallas as pl
from jax.experimental.pallas import tpu as pltpu
from jax.sharding import Mesh
from jax.sharding import PartitionSpec as P


EP = ("ep_0", "ep_1")
GRP_EP = ("grp", "ep_0", "ep_1")
GRP_EP_TP = ("grp", "ep_0", "ep_1", "tp")
LANES = 128
EPSILON = 1e-06


def contract(a, b, dims):
    return lax.dot_general(a, b, (dims, ((), ())), preferred_element_type=jnp.float32)


def attention_kernel(
    steps, head_size, lam_ref, gain_ref, q1_ref, q2_ref, kv_ref, out_ref, q_s, max_s, sum_s, acc_s
):
    step = pl.program_id(0)
    rows, q_width = q1_ref.shape
    heads = q_width // head_size
    value_size = out_ref.shape[1] // heads
    block = kv_ref.shape[0]

    @pl.when(step == 0)
    def _():
        lane_head = lax.broadcasted_iota(jnp.int32, (rows, q_width), 1) // head_size
        for m, q_ref in enumerate((q1_ref, q2_ref)):
            scaled = q_ref[...].astype(jnp.float32) * head_size ** (-0.5)
            for h in range(heads):
                q_s[m * heads + h] = jnp.where(lane_head == h, scaled, 0.0).astype(jnp.bfloat16)
        max_s[...] = jnp.full_like(max_s, -jnp.inf)
        sum_s[...] = jnp.zeros_like(sum_s)
        acc_s[...] = jnp.zeros_like(acc_s)

    for h in range(heads):
        value_from = 2 * q_width + h * value_size
        for m in range(2):
            i = m * heads + h
            scores = contract(q_s[i], kv_ref[:, m * q_width : (m + 1) * q_width], ((1,), (1,)))
            old_max = max_s[i]
            new_max = jnp.maximum(old_max, jnp.max(scores, axis=1, keepdims=True))
            rescale = jnp.exp(old_max - new_max)
            weights = jnp.exp(scores - new_max)
            lane_sum = weights[:, :LANES]
            for j in range(1, block // LANES):
                lane_sum = lane_sum + weights[:, j * LANES : (j + 1) * LANES]
            sum_s[i] = sum_s[i] * rescale + lane_sum
            product = contract(
                weights.astype(jnp.bfloat16),
                kv_ref[:, value_from : value_from + value_size],
                ((1,), (0,)),
            )
            acc_s[i] = acc_s[i] * rescale + product
            max_s[i] = new_max

    @pl.when(step == steps - 1)
    def _():
        for h in range(heads):
            first = acc_s[h] / jnp.sum(sum_s[h], axis=1, keepdims=True)
            second = acc_s[heads + h] / jnp.sum(sum_s[heads + h], axis=1, keepdims=True)
            mixture = first - lam_ref[h] * second
            power = jnp.mean(mixture * mixture, axis=1, keepdims=True)
            normed = mixture * lax.rsqrt(power + EPSILON) * gain_ref[...]
            out_ref[:, h * value_size : (h + 1) * value_size] = normed.astype(jnp.bfloat16)


def attention(q1, q2, kv, lam, gain):
    rows, q_width = q1.shape
    heads = lam.shape[0]
    value_width = heads * gain.shape[0]
    block = 3072
    steps = kv.shape[0] // block
    combos = 2 * heads
    flops = 2 * rows * kv.shape[0] * combos * (q_width // heads + gain.shape[0])
    return pl.pallas_call(
        functools.partial(attention_kernel, steps, q_width // heads),
        grid=(steps,),
        out_shape=jax.ShapeDtypeStruct((rows, value_width), jnp.bfloat16),
        in_specs=[
            pl.BlockSpec(memory_space=pltpu.SMEM),
            pl.BlockSpec((1, gain.shape[0]), lambda i: (0, 0)),
            pl.BlockSpec((rows, q_width), lambda i: (0, 0)),
            pl.BlockSpec((rows, q_width), lambda i: (0, 0)),
            pl.BlockSpec((block, kv.shape[1]), lambda i: (i, 0)),
        ],
        out_specs=pl.BlockSpec((rows, value_width), lambda i: (0, 0)),
        scratch_shapes=[
            pltpu.VMEM((combos, rows, q_width), jnp.bfloat16),
            pltpu.VMEM((combos, rows, 1), jnp.float32),
            pltpu.VMEM((combos, rows, LANES), jnp.float32),
            pltpu.VMEM((combos, rows, gain.shape[0]), jnp.float32),
        ],
        compiler_params=pltpu.CompilerParams(
            dimension_semantics=("arbitrary",), vmem_limit_bytes=48 * 2**20
        ),
        cost_estimate=pl.CostEstimate(
            flops=flops * 4, bytes_accessed=kv.size * 2, transcendentals=rows * kv.shape[0] * combos
        ),
        name="attention",
    )(lam, gain.reshape(1, -1), q1, q2, kv)


def ranked(ids):
    rows, top = ids.shape
    lower = lax.broadcasted_iota(jnp.int32, (rows, rows), 0) >= lax.broadcasted_iota(
        jnp.int32, (rows, rows), 1
    )
    lower = jnp.where(lower, 1.0, 0.0).astype(jnp.bfloat16)
    lane = lax.broadcasted_iota(jnp.int32, (rows, LANES), 1)
    before = jnp.zeros((1, LANES), jnp.float32)
    found = []
    for k in range(top):
        one = ids[:, k : k + 1] == lane
        ones = jnp.where(one, 1.0, 0.0)
        counts = contract(lower, ones.astype(jnp.bfloat16), ((1,), (0,))) + before
        rank = jnp.sum(jnp.where(one, counts, 0.0), axis=1, keepdims=True) - 1.0
        found.append((ids[:, k : k + 1], rank.astype(jnp.int32)))
        before = before + jnp.sum(ones, axis=0, keepdims=True)
    return found


def pack_kernel(
    capacity, core_ref, own_ref, other_ref, own_ids_ref, other_ids_ref, gain_ref,
    packed_ref, normed_ref,
):
    core = core_ref[0]
    slots = packed_ref.shape[0]
    rows = own_ref.shape[0]
    slot_lane = lax.broadcasted_iota(jnp.int32, (rows, slots), 1)
    masks, sources = [], []
    for ref, ids_ref, source in (
        (own_ref, own_ids_ref, core),
        (other_ref, other_ids_ref, 1 - core),
    ):
        wide = ref[...].astype(jnp.float32)
        power = jnp.mean(wide * wide, axis=1, keepdims=True)
        normed = (wide * lax.rsqrt(power + EPSILON) * gain_ref[...]).astype(jnp.bfloat16)
        if ref is own_ref:
            normed_ref[...] = normed
        hit = jnp.zeros((rows, slots), jnp.float32)
        for ids, rank in ranked(ids_ref[...]):
            slot = (ids >> 1) * (2 * capacity) + source * capacity + rank
            slot = jnp.where((ids & 1) == core, slot, -1)
            hit = hit + jnp.where(slot == slot_lane, 1.0, 0.0)
        masks.append(hit.astype(jnp.bfloat16))
        sources.append(normed)
    total = contract(masks[0], sources[0], ((0,), (0,)))
    total = total + contract(masks[1], sources[1], ((0,), (0,)))
    packed_ref[...] = total.astype(jnp.bfloat16)


def pack(core, own, other, own_ids, other_ids, gain, experts, capacity):
    rows, width = own.shape
    slots = experts * capacity
    vmem = pl.BlockSpec(memory_space=pltpu.VMEM)
    return pl.pallas_call(
        functools.partial(pack_kernel, capacity),
        out_shape=(
            jax.ShapeDtypeStruct((slots, width), jnp.bfloat16),
            jax.ShapeDtypeStruct((rows, width), jnp.bfloat16),
        ),
        in_specs=[pl.BlockSpec(memory_space=pltpu.SMEM)] + [vmem] * 5,
        out_specs=(vmem, vmem),
        compiler_params=pltpu.CompilerParams(vmem_limit_bytes=32 * 2**20),
        cost_estimate=pl.CostEstimate(
            flops=4 * slots * rows * width * 8, bytes_accessed=4 * rows * width * 2, transcendentals=0
        ),
        name="pack",
    )(core, own, other, own_ids, other_ids, gain.reshape(1, -1))


def silu_product(gate, up):
    return (gate / (1.0 + jnp.exp(-gate)) * up).astype(jnp.bfloat16)


def experts_kernel(width, gates, ups, downs, array_count, rows_ref, *refs):
    arrays = refs[:array_count]
    out_ref, gate_s, up_s, down_s, hidden_s, wide_sem, down_sem = refs[array_count:]
    parts = len(gates)

    def piece(where):
        return arrays[where[0]].at[where[1:]] if len(where) > 1 else arrays[where[0]]

    copies = []
    for p in range(parts):
        gate = pltpu.make_async_copy(piece(gates[p]), gate_s.at[p], wide_sem.at[0, p])
        up = pltpu.make_async_copy(piece(ups[p]), up_s.at[p], wide_sem.at[1, p])
        gate.start()
        up.start()
        copies.append((gate, up))
    downs_going = []
    at = 0
    for d, where in enumerate(downs):
        ref = piece(where)
        copy = pltpu.make_async_copy(ref, down_s.at[pl.ds(at, ref.shape[0])], down_sem.at[d])
        copy.start()
        downs_going.append(copy)
        at += ref.shape[0]
    for p in range(parts):
        copies[p][0].wait()
        gate = contract(rows_ref[...], gate_s[p], ((1,), (0,)))
        copies[p][1].wait()
        up = contract(rows_ref[...], up_s[p], ((1,), (0,)))
        hidden_s[:, p * width : (p + 1) * width] = silu_product(gate, up)
    for copy in downs_going:
        copy.wait()
    columns = out_ref.shape[1]
    tile = 512
    for c in range(columns // tile):
        piece = contract(hidden_s[...], down_s[:, c * tile : (c + 1) * tile], ((1,), (0,)))
        out_ref[:, c * tile : (c + 1) * tile] = piece.astype(out_ref.dtype)


def run_experts(rows, arrays, gates, ups, downs, width, out_dtype):
    parts = len(gates)
    hidden = parts * width
    model = rows.shape[1]
    hbm = pl.BlockSpec(memory_space=pltpu.MemorySpace.HBM)
    vmem = pl.BlockSpec(memory_space=pltpu.VMEM)
    return pl.pallas_call(
        functools.partial(experts_kernel, width, gates, ups, downs, len(arrays)),
        out_shape=jax.ShapeDtypeStruct(rows.shape, out_dtype),
        in_specs=[vmem] + [hbm] * len(arrays),
        out_specs=vmem,
        scratch_shapes=[
            pltpu.VMEM((parts, model, width), jnp.bfloat16),
            pltpu.VMEM((parts, model, width), jnp.bfloat16),
            pltpu.VMEM((hidden, model), jnp.bfloat16),
            pltpu.VMEM((rows.shape[0], hidden), jnp.bfloat16),
            pltpu.SemaphoreType.DMA((2, parts)),
            pltpu.SemaphoreType.DMA((len(downs),)),
        ],
        compiler_params=pltpu.CompilerParams(vmem_limit_bytes=61 * 2**20),
        cost_estimate=pl.CostEstimate(
            flops=6 * rows.shape[0] * model * hidden * 3,
            bytes_accessed=3 * hidden * model * 2,
            transcendentals=rows.shape[0] * hidden,
        ),
    )(rows, *arrays)


def combine_kernel(
    capacity, core_ref, own_ref, other_ref, ids_ref, weights_ref, shared_ref, out_ref
):
    core = core_ref[0]
    slots = own_ref.shape[0]
    rows = ids_ref.shape[0]
    slot_lane = lax.broadcasted_iota(jnp.int32, (rows, slots), 1)
    total = shared_ref[...]
    for k, (ids, rank) in enumerate(ranked(ids_ref[...])):
        slot = (ids >> 1) * (2 * capacity) + core * capacity + rank
        mine = (ids & 1) == core
        from_own = jnp.where(jnp.where(mine, slot, -1) == slot_lane, 1.0, 0.0)
        from_other = jnp.where(jnp.where(mine, -1, slot) == slot_lane, 1.0, 0.0)
        picked = contract(from_own.astype(jnp.bfloat16), own_ref[...], ((1,), (0,)))
        picked = picked + contract(from_other.astype(jnp.bfloat16), other_ref[...], ((1,), (0,)))
        total = total + weights_ref[:, k : k + 1] * picked
    out_ref[...] = total.astype(jnp.bfloat16)


def combine(core, own, other, ids, weights, shared, capacity):
    vmem = pl.BlockSpec(memory_space=pltpu.VMEM)
    return pl.pallas_call(
        functools.partial(combine_kernel, capacity),
        out_shape=jax.ShapeDtypeStruct(shared.shape, jnp.bfloat16),
        in_specs=[pl.BlockSpec(memory_space=pltpu.SMEM)] + [vmem] * 5,
        out_specs=vmem,
        compiler_params=pltpu.CompilerParams(vmem_limit_bytes=32 * 2**20),
        cost_estimate=pl.CostEstimate(
            flops=8 * own.size * ids.shape[0], bytes_accessed=own.size * 4, transcendentals=0
        ),
        name="combine",
    )(core, own, other, ids, weights, shared)


def shards(
    query_first,
    query_second,
    key_first,
    key_second,
    values,
    lambda_head,
    head_gain,
    out_weight,
    tokens,
    norm_gain,
    expert_ids,
    expert_weights,
    expert_gate,
    expert_up,
    expert_down,
    shared_gate,
    shared_up,
    shared_down,
):
    chips = lax.axis_size("ep_0")
    experts = expert_gate.shape[0] * lax.axis_size(EP)
    row_count, top_count = expert_ids.shape
    capacity = row_count * top_count * 3 // (2 * experts)
    width = tokens.shape[1]
    core = lax.axis_index("ep_1").reshape(1)
    ring = lax.axis_size("tp")
    to_right = [(i, (i + 1) % ring) for i in range(ring)]
    to_left = [(i, (i - 1) % ring) for i in range(ring)]

    def swap(value):
        return lax.ppermute(value, "ep_1", [(0, 1), (1, 0)])

    def right(value):
        return lax.ppermute(value, "tp", to_right)

    def left(value):
        return lax.ppermute(value, "tp", to_left)

    other_tokens = swap(tokens)
    other_ids = swap(expert_ids)

    gate, up, down = expert_gate[0], expert_up[0], expert_down[0]
    gate_l, up_r = right(gate), left(up)
    down_l, down_r = right(down), left(down)
    up_l, gate_r = right(up), left(gate)
    half = down.shape[0] // 2
    gate_o, up_o = right(gate_l), left(up_r)
    down_o1, down_o2 = right(down_l[:half]), left(down_r[half:])

    kv = lax.all_gather(
        jnp.concatenate([key_first, key_second, values], axis=1), EP, axis=0, tiled=True
    )

    packed, normed = pack(
        core, tokens, other_tokens, expert_ids, other_ids, norm_gain, experts, capacity
    )
    chunks = packed.reshape(chips, 2 * capacity, width)
    arrived = lax.all_to_all(chunks, "ep_0", split_axis=0, concat_axis=0, tiled=True)

    shared_both = jnp.concatenate([shared_gate, shared_up], axis=1)
    shared_both, shared_deep, gate_o, up_o, down_o1, down_o2 = lax.optimization_barrier(
        (shared_both, shared_down, gate_o, up_o, down_o1, down_o2)
    )
    shared_wide = lax.all_gather(shared_both, "tp", axis=0, tiled=False)
    shared_deep = lax.all_gather(shared_deep, "tp", axis=0, tiled=False)

    head_rows = attention(query_first, query_second, kv, lambda_head, head_gain)

    routed = run_experts(
        arrived.reshape(-1, width),
        (gate, gate_l, gate_r, gate_o, up, up_l, up_r, up_o)
        + (down, down_l, down_r, down_o1, down_o2),
        ((0,), (1,), (2,), (3,)),
        ((4,), (5,), (6,), (7,)),
        ((8,), (9,), (10,), (11,), (12,)),
        gate.shape[1],
        jnp.bfloat16,
    )
    outgoing = routed.reshape(chips, 2 * capacity, width)
    returned = lax.all_to_all(outgoing, "ep_0", split_axis=0, concat_axis=0, tiled=True)
    returned = returned.reshape(-1, width)

    part = shared_gate.shape[1]
    every = slice(None)
    shared = run_experts(
        normed,
        (shared_wide, shared_deep),
        tuple((0, i, every, pl.ds(0, part)) for i in range(ring)),
        tuple((0, i, every, pl.ds(part, part)) for i in range(ring)),
        tuple((1, i) for i in range(ring)),
        part,
        jnp.float32,
    )
    position_heads = lax.all_to_all(head_rows, "tp", split_axis=0, concat_axis=1, tiled=True)
    mixed = jnp.dot(position_heads, out_weight, preferred_element_type=jnp.float32).astype(
        jnp.bfloat16
    )
    expert_out = combine(
        core, returned, swap(returned), expert_ids, expert_weights, shared, capacity
    )
    return (mixed, expert_out)


def solution(mesh):
    torus = Mesh(
        mesh.devices.reshape(mesh.shape["grp"], mesh.shape["ep"] // 2, 2, mesh.shape["tp"]),
        ("grp", "ep_0", "ep_1", "tp"),
    )
    placed = (
        P(GRP_EP, "tp"),
        P(GRP_EP, "tp"),
        P(GRP_EP, "tp"),
        P(GRP_EP, "tp"),
        P(GRP_EP, "tp"),
        P("tp"),
        P(),
        P(),
        P(GRP_EP_TP, None),
        P(),
        P(GRP_EP_TP, None),
        P(GRP_EP_TP, None),
        P(EP, None, "tp"),
        P(EP, None, "tp"),
        P(EP, "tp", None),
        P(None, "tp"),
        P(None, "tp"),
        P("tp", None),
    )

    return jax.shard_map(
        shards,
        mesh=torus,
        in_specs=placed,
        out_specs=(P(GRP_EP_TP, None), P(GRP_EP_TP, None)),
        check_vma=False,
    )
```

```python
import functools

import jax
import jax.numpy as jnp
from jax import lax
from jax.experimental import pallas as pl
from jax.experimental.pallas import tpu as pltpu
from jax.sharding import Mesh
from jax.sharding import PartitionSpec as P


EP = ("ep_0", "ep_1")
GRP_EP = ("grp", "ep_0", "ep_1")
GRP_EP_TP = ("grp", "ep_0", "ep_1", "tp")
LANES = 128
EPSILON = 1e-06


def contract(a, b, dims):
    return lax.dot_general(a, b, (dims, ((), ())), preferred_element_type=jnp.float32)


def attention_kernel(
    steps, head_size, lam_ref, gain_ref, q1_ref, q2_ref, kv_ref, out_ref, q_s, max_s, sum_s, acc_s
):
    step = pl.program_id(0)
    rows, q_width = q1_ref.shape
    heads = q_width // head_size
    value_size = out_ref.shape[1] // heads
    block = kv_ref.shape[0]

    @pl.when(step == 0)
    def _():
        lane_head = lax.broadcasted_iota(jnp.int32, (rows, q_width), 1) // head_size
        for m, q_ref in enumerate((q1_ref, q2_ref)):
            scaled = q_ref[...].astype(jnp.float32) * head_size ** (-0.5)
            for h in range(heads):
                q_s[m * heads + h] = jnp.where(lane_head == h, scaled, 0.0).astype(jnp.bfloat16)
        max_s[...] = jnp.full_like(max_s, -jnp.inf)
        sum_s[...] = jnp.zeros_like(sum_s)
        acc_s[...] = jnp.zeros_like(acc_s)

    for h in range(heads):
        value_from = 2 * q_width + h * value_size
        for m in range(2):
            i = m * heads + h
            scores = contract(q_s[i], kv_ref[:, m * q_width : (m + 1) * q_width], ((1,), (1,)))
            old_max = max_s[i]
            new_max = jnp.maximum(old_max, jnp.max(scores, axis=1, keepdims=True))
            rescale = jnp.exp(old_max - new_max)
            weights = jnp.exp(scores - new_max)
            lane_sum = weights[:, :LANES]
            for j in range(1, block // LANES):
                lane_sum = lane_sum + weights[:, j * LANES : (j + 1) * LANES]
            sum_s[i] = sum_s[i] * rescale + lane_sum
            product = contract(
                weights.astype(jnp.bfloat16),
                kv_ref[:, value_from : value_from + value_size],
                ((1,), (0,)),
            )
            acc_s[i] = acc_s[i] * rescale + product
            max_s[i] = new_max

    @pl.when(step == steps - 1)
    def _():
        for h in range(heads):
            first = acc_s[h] / jnp.sum(sum_s[h], axis=1, keepdims=True)
            second = acc_s[heads + h] / jnp.sum(sum_s[heads + h], axis=1, keepdims=True)
            mixture = first - lam_ref[h] * second
            power = jnp.mean(mixture * mixture, axis=1, keepdims=True)
            normed = mixture * lax.rsqrt(power + EPSILON) * gain_ref[...]
            out_ref[:, h * value_size : (h + 1) * value_size] = normed.astype(jnp.bfloat16)


def attention(q1, q2, kv, lam, gain):
    rows, q_width = q1.shape
    heads = lam.shape[0]
    value_width = heads * gain.shape[0]
    block = 3072
    steps = kv.shape[0] // block
    combos = 2 * heads
    flops = 2 * rows * kv.shape[0] * combos * (q_width // heads + gain.shape[0])
    return pl.pallas_call(
        functools.partial(attention_kernel, steps, q_width // heads),
        grid=(steps,),
        out_shape=jax.ShapeDtypeStruct((rows, value_width), jnp.bfloat16),
        in_specs=[
            pl.BlockSpec(memory_space=pltpu.SMEM),
            pl.BlockSpec((1, gain.shape[0]), lambda i: (0, 0)),
            pl.BlockSpec((rows, q_width), lambda i: (0, 0)),
            pl.BlockSpec((rows, q_width), lambda i: (0, 0)),
            pl.BlockSpec((block, kv.shape[1]), lambda i: (i, 0)),
        ],
        out_specs=pl.BlockSpec((rows, value_width), lambda i: (0, 0)),
        scratch_shapes=[
            pltpu.VMEM((combos, rows, q_width), jnp.bfloat16),
            pltpu.VMEM((combos, rows, 1), jnp.float32),
            pltpu.VMEM((combos, rows, LANES), jnp.float32),
            pltpu.VMEM((combos, rows, gain.shape[0]), jnp.float32),
        ],
        compiler_params=pltpu.CompilerParams(
            dimension_semantics=("arbitrary",), vmem_limit_bytes=48 * 2**20
        ),
        cost_estimate=pl.CostEstimate(
            flops=flops * 4, bytes_accessed=kv.size * 2, transcendentals=rows * kv.shape[0] * combos
        ),
        name="attention",
    )(lam, gain.reshape(1, -1), q1, q2, kv)


def ranked(ids):
    rows, top = ids.shape
    lower = lax.broadcasted_iota(jnp.int32, (rows, rows), 0) >= lax.broadcasted_iota(
        jnp.int32, (rows, rows), 1
    )
    lower = jnp.where(lower, 1.0, 0.0).astype(jnp.bfloat16)
    lane = lax.broadcasted_iota(jnp.int32, (rows, LANES), 1)
    before = jnp.zeros((1, LANES), jnp.float32)
    found = []
    for k in range(top):
        one = ids[:, k : k + 1] == lane
        ones = jnp.where(one, 1.0, 0.0)
        counts = contract(lower, ones.astype(jnp.bfloat16), ((1,), (0,))) + before
        rank = jnp.sum(jnp.where(one, counts, 0.0), axis=1, keepdims=True) - 1.0
        found.append((ids[:, k : k + 1], rank.astype(jnp.int32)))
        before = before + jnp.sum(ones, axis=0, keepdims=True)
    return found


def pack_kernel(
    capacity, core_ref, own_ref, other_ref, own_ids_ref, other_ids_ref, gain_ref,
    packed_ref, normed_ref,
):
    core = core_ref[0]
    slots = packed_ref.shape[0]
    rows = own_ref.shape[0]
    slot_lane = lax.broadcasted_iota(jnp.int32, (rows, slots), 1)
    masks, sources = [], []
    for ref, ids_ref, source in (
        (own_ref, own_ids_ref, core),
        (other_ref, other_ids_ref, 1 - core),
    ):
        wide = ref[...].astype(jnp.float32)
        power = jnp.mean(wide * wide, axis=1, keepdims=True)
        normed = (wide * lax.rsqrt(power + EPSILON) * gain_ref[...]).astype(jnp.bfloat16)
        if ref is own_ref:
            normed_ref[...] = normed
        hit = jnp.zeros((rows, slots), jnp.float32)
        for ids, rank in ranked(ids_ref[...]):
            slot = (ids >> 1) * (2 * capacity) + source * capacity + rank
            slot = jnp.where((ids & 1) == core, slot, -1)
            hit = hit + jnp.where(slot == slot_lane, 1.0, 0.0)
        masks.append(hit.astype(jnp.bfloat16))
        sources.append(normed)
    total = contract(masks[0], sources[0], ((0,), (0,)))
    total = total + contract(masks[1], sources[1], ((0,), (0,)))
    packed_ref[...] = total.astype(jnp.bfloat16)


def pack(core, own, other, own_ids, other_ids, gain, experts, capacity):
    rows, width = own.shape
    slots = experts * capacity
    vmem = pl.BlockSpec(memory_space=pltpu.VMEM)
    return pl.pallas_call(
        functools.partial(pack_kernel, capacity),
        out_shape=(
            jax.ShapeDtypeStruct((slots, width), jnp.bfloat16),
            jax.ShapeDtypeStruct((rows, width), jnp.bfloat16),
        ),
        in_specs=[pl.BlockSpec(memory_space=pltpu.SMEM)] + [vmem] * 5,
        out_specs=(vmem, vmem),
        compiler_params=pltpu.CompilerParams(vmem_limit_bytes=32 * 2**20),
        cost_estimate=pl.CostEstimate(
            flops=4 * slots * rows * width * 8, bytes_accessed=4 * rows * width * 2, transcendentals=0
        ),
        name="pack",
    )(core, own, other, own_ids, other_ids, gain.reshape(1, -1))


def silu_product(gate, up):
    return (gate / (1.0 + jnp.exp(-gate)) * up).astype(jnp.bfloat16)


def experts_kernel(width, gates, ups, downs, array_count, rows_ref, *refs):
    arrays = refs[:array_count]
    out_ref, gate_s, up_s, down_s, hidden_s, wide_sem, down_sem = refs[array_count:]
    parts = len(gates)

    def piece(where):
        return arrays[where[0]].at[where[1:]] if len(where) > 1 else arrays[where[0]]

    copies = []
    for p in range(parts):
        gate = pltpu.make_async_copy(piece(gates[p]), gate_s.at[p], wide_sem.at[0, p])
        up = pltpu.make_async_copy(piece(ups[p]), up_s.at[p], wide_sem.at[1, p])
        gate.start()
        up.start()
        copies.append((gate, up))
    downs_going = []
    at = 0
    for d, where in enumerate(downs):
        ref = piece(where)
        copy = pltpu.make_async_copy(ref, down_s.at[pl.ds(at, ref.shape[0])], down_sem.at[d])
        copy.start()
        downs_going.append(copy)
        at += ref.shape[0]
    for p in range(parts):
        copies[p][0].wait()
        gate = contract(rows_ref[...], gate_s[p], ((1,), (0,)))
        copies[p][1].wait()
        up = contract(rows_ref[...], up_s[p], ((1,), (0,)))
        hidden_s[:, p * width : (p + 1) * width] = silu_product(gate, up)
    for copy in downs_going:
        copy.wait()
    columns = out_ref.shape[1]
    tile = 512
    for c in range(columns // tile):
        piece = contract(hidden_s[...], down_s[:, c * tile : (c + 1) * tile], ((1,), (0,)))
        out_ref[:, c * tile : (c + 1) * tile] = piece.astype(out_ref.dtype)


def run_experts(rows, arrays, gates, ups, downs, width, out_dtype):
    parts = len(gates)
    hidden = parts * width
    model = rows.shape[1]
    hbm = pl.BlockSpec(memory_space=pltpu.MemorySpace.HBM)
    vmem = pl.BlockSpec(memory_space=pltpu.VMEM)
    return pl.pallas_call(
        functools.partial(experts_kernel, width, gates, ups, downs, len(arrays)),
        out_shape=jax.ShapeDtypeStruct(rows.shape, out_dtype),
        in_specs=[vmem] + [hbm] * len(arrays),
        out_specs=vmem,
        scratch_shapes=[
            pltpu.VMEM((parts, model, width), jnp.bfloat16),
            pltpu.VMEM((parts, model, width), jnp.bfloat16),
            pltpu.VMEM((hidden, model), jnp.bfloat16),
            pltpu.VMEM((rows.shape[0], hidden), jnp.bfloat16),
            pltpu.SemaphoreType.DMA((2, parts)),
            pltpu.SemaphoreType.DMA((len(downs),)),
        ],
        compiler_params=pltpu.CompilerParams(vmem_limit_bytes=61 * 2**20),
        cost_estimate=pl.CostEstimate(
            flops=6 * rows.shape[0] * model * hidden * 3,
            bytes_accessed=3 * hidden * model * 2,
            transcendentals=rows.shape[0] * hidden,
        ),
    )(rows, *arrays)


def combine_kernel(
    capacity, core_ref, own_ref, other_ref, ids_ref, weights_ref, shared_ref, out_ref
):
    core = core_ref[0]
    slots = own_ref.shape[0]
    rows = ids_ref.shape[0]
    slot_lane = lax.broadcasted_iota(jnp.int32, (rows, slots), 1)
    total = shared_ref[...]
    for k, (ids, rank) in enumerate(ranked(ids_ref[...])):
        slot = (ids >> 1) * (2 * capacity) + core * capacity + rank
        mine = (ids & 1) == core
        from_own = jnp.where(jnp.where(mine, slot, -1) == slot_lane, 1.0, 0.0)
        from_other = jnp.where(jnp.where(mine, -1, slot) == slot_lane, 1.0, 0.0)
        picked = contract(from_own.astype(jnp.bfloat16), own_ref[...], ((1,), (0,)))
        picked = picked + contract(from_other.astype(jnp.bfloat16), other_ref[...], ((1,), (0,)))
        total = total + weights_ref[:, k : k + 1] * picked
    out_ref[...] = total.astype(jnp.bfloat16)


def combine(core, own, other, ids, weights, shared, capacity):
    vmem = pl.BlockSpec(memory_space=pltpu.VMEM)
    return pl.pallas_call(
        functools.partial(combine_kernel, capacity),
        out_shape=jax.ShapeDtypeStruct(shared.shape, jnp.bfloat16),
        in_specs=[pl.BlockSpec(memory_space=pltpu.SMEM)] + [vmem] * 5,
        out_specs=vmem,
        compiler_params=pltpu.CompilerParams(vmem_limit_bytes=32 * 2**20),
        cost_estimate=pl.CostEstimate(
            flops=8 * own.size * ids.shape[0], bytes_accessed=own.size * 4, transcendentals=0
        ),
        name="combine",
    )(core, own, other, ids, weights, shared)


def shards(
    query_first,
    query_second,
    key_first,
    key_second,
    values,
    lambda_head,
    head_gain,
    out_weight,
    tokens,
    norm_gain,
    expert_ids,
    expert_weights,
    expert_gate,
    expert_up,
    expert_down,
    shared_gate,
    shared_up,
    shared_down,
):
    chips = lax.axis_size("ep_0")
    experts = expert_gate.shape[0] * lax.axis_size(EP)
    row_count, top_count = expert_ids.shape
    capacity = row_count * top_count * 3 // (2 * experts)
    width = tokens.shape[1]
    core = lax.axis_index("ep_1").reshape(1)
    ring = lax.axis_size("tp")
    to_right = [(i, (i + 1) % ring) for i in range(ring)]
    to_left = [(i, (i - 1) % ring) for i in range(ring)]

    def swap(value):
        return lax.ppermute(value, "ep_1", [(0, 1), (1, 0)])

    def right(value):
        return lax.ppermute(value, "tp", to_right)

    def left(value):
        return lax.ppermute(value, "tp", to_left)

    other_tokens = swap(tokens)
    other_ids = swap(expert_ids)

    gate, up, down = expert_gate[0], expert_up[0], expert_down[0]
    gate_l, up_r = right(gate), left(up)
    down_l, down_r = right(down), left(down)
    up_l, gate_r = right(up), left(gate)
    half = down.shape[0] // 2
    gate_o, up_o = right(gate_l), left(up_r)
    down_o1, down_o2 = right(down_l[:half]), left(down_r[half:])

    kv = lax.all_gather(
        jnp.concatenate([key_first, key_second, values], axis=1), EP, axis=0, tiled=True
    )

    packed, normed = pack(
        core, tokens, other_tokens, expert_ids, other_ids, norm_gain, experts, capacity
    )
    chunks = packed.reshape(chips, 2 * capacity, width)
    arrived = lax.all_to_all(chunks, "ep_0", split_axis=0, concat_axis=0, tiled=True)

    both = jnp.concatenate([shared_gate, shared_up], axis=1)
    both_l, both_r, deep_l, deep_r = right(both), left(both), right(shared_down), left(shared_down)
    both_o, deep_o = right(both_l), left(deep_r)

    head_rows = attention(query_first, query_second, kv, lambda_head, head_gain)

    routed = run_experts(
        arrived.reshape(-1, width),
        (gate, gate_l, gate_r, gate_o, up, up_l, up_r, up_o)
        + (down, down_l, down_r, down_o1, down_o2),
        ((0,), (1,), (2,), (3,)),
        ((4,), (5,), (6,), (7,)),
        ((8,), (9,), (10,), (11,), (12,)),
        gate.shape[1],
        jnp.bfloat16,
    )
    outgoing = routed.reshape(chips, 2 * capacity, width)
    returned = lax.all_to_all(outgoing, "ep_0", split_axis=0, concat_axis=0, tiled=True)
    returned = returned.reshape(-1, width)

    part = shared_gate.shape[1]
    every = slice(None)
    shared = run_experts(
        normed,
        (both, both_l, both_r, both_o, shared_down, deep_l, deep_r, deep_o),
        tuple((i, every, pl.ds(0, part)) for i in range(ring)),
        tuple((i, every, pl.ds(part, part)) for i in range(ring)),
        tuple((ring + i,) for i in range(ring)),
        part,
        jnp.float32,
    )
    position_heads = lax.all_to_all(head_rows, "tp", split_axis=0, concat_axis=1, tiled=True)
    mixed = jnp.dot(position_heads, out_weight, preferred_element_type=jnp.float32).astype(
        jnp.bfloat16
    )
    expert_out = combine(
        core, returned, swap(returned), expert_ids, expert_weights, shared, capacity
    )
    return (mixed, expert_out)


def solution(mesh):
    torus = Mesh(
        mesh.devices.reshape(mesh.shape["grp"], mesh.shape["ep"] // 2, 2, mesh.shape["tp"]),
        ("grp", "ep_0", "ep_1", "tp"),
    )
    placed = (
        P(GRP_EP, "tp"),
        P(GRP_EP, "tp"),
        P(GRP_EP, "tp"),
        P(GRP_EP, "tp"),
        P(GRP_EP, "tp"),
        P("tp"),
        P(),
        P(),
        P(GRP_EP_TP, None),
        P(),
        P(GRP_EP_TP, None),
        P(GRP_EP_TP, None),
        P(EP, None, "tp"),
        P(EP, None, "tp"),
        P(EP, "tp", None),
        P(None, "tp"),
        P(None, "tp"),
        P("tp", None),
    )

    return jax.shard_map(
        shards,
        mesh=torus,
        in_specs=placed,
        out_specs=(P(GRP_EP_TP, None), P(GRP_EP_TP, None)),
        check_vma=False,
    )
```
